32 devices in a mesh: ep: 8 (over z, x), tp: 4 (over y, core).
Axes of the slice: x: 2, y: 2, z: 4, core: 2. Of those that a mesh axis runs over, the one named last changes fastest.
Arguments:
- query_logits: bfloat16 [2048, 2048], P('ep', 'tp'), may hold values from -6 to 6
- forget_gate_logits: bfloat16 [2048, 2048], P('ep', 'tp'), may hold values from -3.75 to 3.75
- written_values: bfloat16 [2048, 2048], P('ep', 'tp'), may hold values from -6 to 6
- output_gate_logits: bfloat16 [2048, 2048], P('ep', 'tp'), may hold values from -6 to 6
- gap: float32 [2048], P('tp'), may hold values from 4.8828125e-05 to 0.06
- extra_log_forget: float32 [2048, 2048], P('ep', 'tp'), may hold values from -0.7 to 0
- head_norm_scale: float32 [2048], P('tp'), may hold values from 0.1 to 1.9
- mixer_output_matrix: bfloat16 [2048, 2048], P('tp'), may hold values from -0.125 to 0.125
- expert_input_tokens: bfloat16 [2048, 2048], P('ep'), may hold values from -12 to 12
- expert_norm_scale: float32 [2048], replicated, may hold values from 0.1 to 1.9
- routes: int32 [2048, 2], P('ep'), may hold values from 0 to 7, all different within a row; in each aligned block of 256 rows (0 to 255, 256 to 511, ...) at most 96 rows name the same one
- router_scores_chosen: float32 [2048, 2], P('ep'), may hold values from -6 to 6
- expert_gate_matrix: bfloat16 [8, 2048, 4096], P('ep', None, 'tp'), may hold values from -0.125 to 0.125
- expert_up_matrix: bfloat16 [8, 2048, 4096], P('ep', None, 'tp'), may hold values from -0.125 to 0.125
- expert_down_matrix: bfloat16 [8, 2048, 4096], P('ep', None, 'tp'), may hold values from -0.09375 to 0.09375
Outputs:
- mixer_output_rows: bfloat16 [2048, 2048], P(('ep', 'tp'))
- expert_out: bfloat16 [2048, 2048], P('ep', 'tp')
The draws below stay inside these ranges and needn't reach their ends.
Inputs may be any that keep to these rules, and one draw needn't show every extreme that they name: `routes`: each row names two different experts. Among the rows of one device no expert is named more than 96 times, and 96 is reached in some blocks.
All inputs are finite; a program needn't handle non-finite values.
Results may differ from the reference program's by a relative error of at most 0.019.
Values may be sent and summed in bfloat16 or wider, within the bound.
No kernel may reach another device: no remote copies, remote signals or barrier semaphores. Data moves between devices by JAX's collectives and lax.ppermute only.
A program may use at most 64 MiB of HBM per device.

```python
import math
import jax
import jax.numpy as jnp
import numpy as np
from jax import lax

HEAD_DIM = 128
HEADS = 16
D = 2048
FF = 4096
TOK_A = 256
TOK_B = 256
TOKENS_A = 2048
TOKENS_B = 2048
EXPERTS = 8
CAP = 96
N_EP = 8
N_TP = 4


def draw_gap(key, part):
    choose_key, lasting_key, quick_key = jax.random.split(jax.random.fold_in(key, 11), 3)
    quick_heads = jax.random.uniform(choose_key, (HEADS,)) < 0.5
    lasting = jnp.exp(jax.random.uniform(lasting_key, (HEADS, HEAD_DIM), jnp.float32, math.log(0.1 / TOKENS_A), math.log(1.0 / TOKENS_A)))
    quick = jnp.exp(jax.random.uniform(quick_key, (HEADS, HEAD_DIM), jnp.float32, math.log(0.02), math.log(0.06)))
    return jnp.where(quick_heads[:, None], quick, lasting).reshape(D).astype(jnp.float32)


def draw_forget_gate_logits(key, part):
    noise_key, shift_key = jax.random.split(jax.random.fold_in(key, 23), 2)
    block_shift = jax.random.uniform(shift_key, (N_EP,), jnp.float32, -1.2, 1.2)
    noise = jnp.clip(jax.random.normal(noise_key, (TOKENS_A, D), jnp.float32), -2.5, 2.5)
    return (noise + jnp.repeat(block_shift, TOK_A)[:, None]).astype(jnp.bfloat16)


def draw_extra_log_forget(key, part):
    where_key, depth_key = jax.random.split(jax.random.fold_in(key, 37), 2)
    spots = jax.random.randint(where_key, (3,), 0, TOKENS_A)
    struck = jnp.any(jnp.arange(TOKENS_A)[:, None] == spots[None, :], axis=1)
    depth = jnp.log(jax.random.uniform(depth_key, (TOKENS_A, D), jnp.float32, 0.5, 0.8))
    return jnp.where(struck[:, None], depth, 0.0).astype(jnp.float32)


def draw_expert_input_tokens(key, part):
    noise_key, scale_key = jax.random.split(jax.random.fold_in(key, 41), 2)
    scales = jnp.exp(jax.random.uniform(scale_key, (TOKENS_B, 1), jnp.float32, math.log(0.3), math.log(3.0)))
    noise = jnp.clip(jax.random.normal(noise_key, (TOKENS_B, D), jnp.float32), -4.0, 4.0)
    return (noise * scales).astype(jnp.bfloat16)


def block_levels(rng, dims, pieces, least, high):
    gain, own = 1.0, jax.random.fold_in(rng, 6)
    for dim, parts in pieces:
        steps = jnp.exp(jax.random.uniform(jax.random.fold_in(own, dim), (parts,), jnp.float32, least / len(pieces), high / len(pieces)))
        gain = gain * jnp.repeat(steps, dims[dim] // parts).reshape([-1 if axis == dim else 1 for axis in range(len(dims))])
    return gain


def deal_out(rng, own, number, rows, amount, top, most, skew):
    ranking = jax.random.permutation(rng, amount)
    crowded, ordinary = shares(amount, rows * top, most, skew, True), shares(amount, rows * top, most, skew, False)
    places = jnp.arange(amount)

    def named(sizes, offset_by):
        used = int((sizes > 0).sum())
        fixed = max(1, used // 4)
        passed = fixed + (places - fixed + offset_by * (used - fixed)) % max(1, amount - fixed)
        return jnp.zeros((amount,), jnp.int32).at[ranking[jnp.where(places < fixed, places, passed)]].set(jnp.asarray(sizes, jnp.int32))

    sizes = jnp.where(number % 4 == 0, named(crowded, number // 4), named(ordinary, number - number // 4 - 1))
    mixed = jax.random.permutation(jax.random.fold_in(own, 3), amount)
    source_of, taker = mixed[0:amount // 2 * 2:2], mixed[1:amount // 2 * 2:2]
    room = jnp.minimum(sizes[source_of] - 1, most - sizes[taker]) // 2
    room = jnp.where((source_of == ranking[0]) | (taker == ranking[0]) | (sizes[taker] == 0), 0, jnp.maximum(room, 0))
    passed = jax.random.randint(jax.random.fold_in(own, 4), (amount // 2,), 0, 1 << 20) % (room + 1)
    sizes = sizes.at[source_of].add(-passed).at[taker].add(passed)
    members = jnp.searchsorted(jnp.cumsum(sizes), jnp.arange(rows * top), side="right").astype(jnp.int32)
    table = members.reshape(top, rows).T
    table = table[jax.random.permutation(jax.random.fold_in(own, 1), rows)]
    offset_by = jax.random.randint(jax.random.fold_in(own, 2), (rows, 1), 0, top)
    return jnp.take_along_axis(table, (jnp.arange(top)[None, :] + offset_by) % top, axis=1)


def shares(number_of, total, limit, skew, full):
    portions = [(1 << 20) // math.isqrt(standing ** skew) + 1 for standing in range(1, number_of + 1)]
    largest = limit if full else min(limit, max(-(-total // number_of), total * portions[0] // sum(portions)))
    least = 1 if total - largest >= number_of - 1 else 0
    counts, spare = [largest] + [least] * (number_of - 1), total - largest - least * (number_of - 1)
    while spare > 0:
        free = [i for i in range(1, number_of) if counts[i] < largest] or [i for i in range(1, number_of) if counts[i] < limit]
        mass, left = sum([portions[i] for i in free]), spare
        for i in free:
            extra = min(limit - counts[i], max(1, left * portions[i] // mass), spare)
            counts[i] = counts[i] + extra
            spare = spare - extra
    return np.array(counts)


def gaussian(stream_key, shape, deviation, limit, shards=(), kind=jnp.bfloat16):
    loudness = block_levels(stream_key, shape, shards, -0.22, 0.18) if shards else 1.0
    drawn = jax.random.normal(stream_key, shape, jnp.float32) * deviation * loudness
    return jnp.minimum(jnp.maximum(drawn, -limit), limit).astype(kind)


def setup_inputs(seed: int = 0) -> dict:
    streams_of = jax.random.split(jax.random.key(seed), 16)
    query_logits = gaussian(streams_of[0], (TOKENS_A, D), 1.0, 6.0, ((0, 8), (1, 4)))
    forget_gate_logits = draw_forget_gate_logits(jax.random.fold_in(streams_of[15], 71), 0)
    written_values = gaussian(streams_of[2], (TOKENS_A, D), 1.0, 6.0, ((0, 8), (1, 4)))
    output_gate_logits = gaussian(streams_of[3], (TOKENS_A, D), 1.0, 6.0, ((0, 8), (1, 4)))
    gap = draw_gap(jax.random.fold_in(streams_of[15], 71), 0)
    extra_log_forget = draw_extra_log_forget(jax.random.fold_in(streams_of[15], 71), 0)
    head_norm_scale = jnp.clip(1.0 + 0.18 * jax.random.normal(streams_of[6], (D,), jnp.float32), 0.1, 1.9)
    mixer_output_matrix = gaussian(streams_of[7], (D, D), D ** -0.5, 0.125, ((0, 4),))
    expert_input_tokens = draw_expert_input_tokens(jax.random.fold_in(streams_of[15], 71), 0)
    expert_norm_scale = jnp.clip(1.0 + 0.18 * jax.random.normal(streams_of[9], (D,), jnp.float32), 0.1, 1.9)
    routes_keys = jax.random.split(jax.random.fold_in(streams_of[10], 1), TOKENS_B // TOK_B)
    routes_turns = jax.random.permutation(jax.random.fold_in(streams_of[10], 3), TOKENS_B // TOK_B)
    routes = jax.vmap(lambda own, number: deal_out(jax.random.fold_in(streams_of[10], 2), own, number, TOK_B, EXPERTS, 2, CAP, 2))(routes_keys, routes_turns).reshape((TOKENS_B, 2))
    router_scores_chosen = gaussian(streams_of[11], (TOKENS_B, 2), 1.5, 6.0, ((0, 8),), jnp.float32)
    expert_gate_matrix = gaussian(streams_of[12], (EXPERTS, D, FF), D ** -0.5, 0.125, ((0, 8), (2, 4)))
    expert_up_matrix = gaussian(streams_of[13], (EXPERTS, D, FF), D ** -0.5, 0.125, ((0, 8), (2, 4)))
    expert_down_matrix = gaussian(streams_of[14], (EXPERTS, D, FF), FF ** -0.5, 0.09375, ((0, 8), (2, 4)))
    return {"query_logits": query_logits, "forget_gate_logits": forget_gate_logits, "written_values": written_values, "output_gate_logits": output_gate_logits, "gap": gap, "extra_log_forget": extra_log_forget, "head_norm_scale": head_norm_scale, "mixer_output_matrix": mixer_output_matrix, "expert_input_tokens": expert_input_tokens, "expert_norm_scale": expert_norm_scale, "routes": routes, "router_scores_chosen": router_scores_chosen, "expert_gate_matrix": expert_gate_matrix, "expert_up_matrix": expert_up_matrix, "expert_down_matrix": expert_down_matrix}


exact_precision = lax.Precision.HIGHEST

def recurrent_portion(query_logits, forget_gate_logits, written_values, output_gate_logits, gap, extra_log_forget, head_norm_scale, mixer_output_matrix):
    final_result = gap * jax.nn.sigmoid(-forget_gate_logits.astype(jnp.float32))
    decay_logarithm = jnp.log1p(-final_result) + extra_log_forget
    queries = jax.nn.silu(query_logits.astype(jnp.float32))
    values = written_values.astype(jnp.float32)

    def by_head(array):
        return array.reshape(TOKENS_A, HEADS, HEAD_DIM)

    def advance(state, inputs):
        query_now, key_now, value_now, decay_now = inputs
        state = jnp.exp(decay_now)[:, :, None] * state + key_now[:, :, None] * value_now[:, None, :]
        output = jnp.einsum('hd,hdv->hv', query_now, state, precision=exact_precision)
        return (state, output)
    start_state = jnp.zeros((HEADS, HEAD_DIM, HEAD_DIM), jnp.float32)
    _, recurrent = lax.scan(advance, start_state, (by_head(queries), by_head(final_result), by_head(values), by_head(decay_logarithm)))
    scaled = recurrent * lax.rsqrt(lax.optimization_barrier(jnp.mean(recurrent * recurrent, axis=-1, keepdims=True)) + 1e-06)
    scaled = scaled.reshape(TOKENS_A, D)
    hidden = (scaled * head_norm_scale * jax.nn.silu(output_gate_logits.astype(jnp.float32))).astype(jnp.bfloat16)
    group_width = D // N_TP

    def add_group(totals, index):
        columns = lax.dynamic_slice_in_dim(hidden, index * group_width, group_width, 1)
        weight_rows = lax.dynamic_slice_in_dim(mixer_output_matrix, index * group_width, group_width, 0)
        partial_sum = jnp.dot(columns, weight_rows, preferred_element_type=jnp.float32)
        rounded = lax.optimization_barrier(partial_sum.astype(jnp.bfloat16)).astype(jnp.float32)
        return (totals + rounded, None)
    mixed_total, _ = lax.scan(add_group, jnp.zeros((TOKENS_A, D), jnp.float32), jnp.arange(N_TP, dtype=jnp.int32))
    return mixed_total.astype(jnp.bfloat16)

def expert_part(expert_input_tokens, expert_norm_scale, routes, router_scores_chosen, expert_gate_matrix, expert_up_matrix, expert_down_matrix):
    inputs32 = expert_input_tokens.astype(jnp.float32)
    centred = inputs32 - lax.optimization_barrier(jnp.mean(inputs32, axis=-1, keepdims=True))
    variance = lax.optimization_barrier(jnp.mean(centred * centred, axis=-1, keepdims=True))
    normed = (centred * lax.rsqrt(variance + 1e-05) * expert_norm_scale).astype(jnp.bfloat16)
    first_weight = jax.nn.sigmoid(router_scores_chosen[:, 0] - router_scores_chosen[:, 1])
    route_weight = jnp.stack([first_weight, 1.0 - first_weight], axis=1)
    flat_routes = routes.reshape(N_EP, TOK_B * 2)
    onehot = (flat_routes[:, :, None] == jnp.arange(EXPERTS, dtype=jnp.int32)[None, None, :]).astype(jnp.int32)
    earlier = jnp.cumsum(onehot, axis=1) - onehot
    position = lax.optimization_barrier(jnp.sum(earlier * onehot, axis=2))
    slot_count = N_EP * CAP
    source = jnp.arange(N_EP, dtype=jnp.int32)[:, None]
    target = (flat_routes * slot_count + source * CAP + position).reshape(-1).astype(jnp.int32)
    token_ids = jnp.arange(TOKENS_B * 2, dtype=jnp.int32) // 2
    owner = jnp.zeros((EXPERTS * slot_count,), jnp.int32).at[target].set(token_ids)
    filled = jnp.zeros((EXPERTS * slot_count,), jnp.bool_).at[target].set(True)
    group_width = FF // N_TP

    def one_expert(unused, inputs):
        owner_ids, live_slots, gate_w, up_w, down_w = inputs
        picked = jnp.where(live_slots[:, None], normed[owner_ids], jnp.zeros((), jnp.bfloat16))
        gate_act = jnp.dot(picked, gate_w, preferred_element_type=jnp.float32)
        up_act = jnp.dot(picked, up_w, preferred_element_type=jnp.float32)
        hidden = (jax.nn.silu(gate_act) * up_act).astype(jnp.bfloat16)

        def add_group(totals, index):
            hidden_cols = lax.dynamic_slice_in_dim(hidden, index * group_width, group_width, 1)
            down_cols = lax.dynamic_slice_in_dim(down_w, index * group_width, group_width, 1)
            partial_sum = lax.dot_general(hidden_cols, down_cols, (((1,), (1,)), ((), ())), preferred_element_type=jnp.float32)
            rounded = lax.optimization_barrier(partial_sum.astype(jnp.bfloat16)).astype(jnp.float32)
            return (totals + rounded, None)
        summed, _ = lax.scan(add_group, jnp.zeros((slot_count, D), jnp.float32), jnp.arange(N_TP, dtype=jnp.int32))
        return (unused, summed.astype(jnp.bfloat16))
    _, results = lax.scan(one_expert, None, (owner.reshape(EXPERTS, slot_count), filled.reshape(EXPERTS, slot_count), expert_gate_matrix, expert_up_matrix, expert_down_matrix))
    chosen = results.reshape(EXPERTS * slot_count, D)[target].astype(jnp.float32).reshape(TOKENS_B, 2, D)
    return lax.optimization_barrier(jnp.sum(chosen * route_weight[:, :, None], axis=1)).astype(jnp.bfloat16)

def reference(query_logits, forget_gate_logits, written_values, output_gate_logits, gap, extra_log_forget, head_norm_scale, mixer_output_matrix, expert_input_tokens, expert_norm_scale, routes, router_scores_chosen, expert_gate_matrix, expert_up_matrix, expert_down_matrix):
    mixer_output_rows = recurrent_portion(query_logits, forget_gate_logits, written_values, output_gate_logits, gap, extra_log_forget, head_norm_scale, mixer_output_matrix)
    expert_out = expert_part(expert_input_tokens, expert_norm_scale, routes, router_scores_chosen, expert_gate_matrix, expert_up_matrix, expert_down_matrix)
    return (mixer_output_rows, expert_out)
```

```python
import functools

import jax
import jax.numpy as jnp
from jax import lax
from jax.experimental import pallas as pl
from jax.experimental.pallas import tpu as pltpu
from jax.sharding import PartitionSpec as P

HEAD_DIM = 128
SPAN = 128
CHUNKS = 1
f32, bf16 = jnp.float32, jnp.bfloat16
NT = (((1,), (1,)), ((), ()))
TN = (((0,), (0,)), ((), ()))


def dot(a, b, dims=(((1,), (0,)), ((), ())), precision=None):
    return lax.dot_general(a, b, dims, precision=precision, preferred_element_type=f32)


def sigmoid(v):
    return 1.0 / (1.0 + jnp.exp(-v))


def mixer_local(q_ref, f_ref, v_ref, extra_ref, gap_ref, within_ref, qdec_ref, packed_ref):
    tokens, channels = q_ref.shape
    row = lax.broadcasted_iota(jnp.int32, (SPAN, SPAN), 0)
    col = lax.broadcasted_iota(jnp.int32, (SPAN, SPAN), 1)
    causal = row >= col
    lower = causal.astype(f32)
    heads = channels // HEAD_DIM
    state = [None] * heads
    total_before = jnp.zeros((1, channels), f32)
    for c in range(tokens // SPAN):
        rows = slice(c * SPAN, (c + 1) * SPAN)
        key = gap_ref[...] * sigmoid(-f_ref[rows, :].astype(f32))
        decay = jnp.log1p(-key) + extra_ref[rows, :]
        run = dot(lower, decay, precision=lax.Precision.HIGHEST)
        middle, total = run[SPAN // 2 - 1 : SPAN // 2, :], run[SPAN - 1 :, :]
        q32 = q_ref[rows, :].astype(f32)
        query = q32 * sigmoid(q32)
        q_mid = (query * jnp.exp(run - middle)).astype(bf16)
        k_mid = (key * jnp.exp(middle - run)).astype(bf16)
        q_run = query * jnp.exp(run)
        k_end = (key * jnp.exp(total - run)).astype(bf16)
        qdec_ref[rows, :] = (q_run * jnp.exp(total_before)).astype(bf16)
        q_run = q_run.astype(bf16)
        gone = jnp.exp(total)
        values = v_ref[rows, :]
        for h in range(heads):
            lanes = slice(h * HEAD_DIM, (h + 1) * HEAD_DIM)
            vh = values[:, lanes]
            scores = jnp.where(causal, dot(q_mid[:, lanes], k_mid[:, lanes], NT), 0.0)
            within = dot(scores.astype(bf16), vh)
            added = dot(vh, k_end[:, lanes], TN)
            if c:
                within = within + dot(q_run[:, lanes], state[h].astype(bf16), NT)
                state[h] = state[h] * gone[:, lanes] + added
            else:
                state[h] = added
            within_ref[rows, lanes] = within
        total_before = total_before + total
    span_decay = jnp.exp(total_before)
    extra_rows = packed_ref.shape[1] - HEAD_DIM
    for h in range(heads):
        lanes = slice(h * HEAD_DIM, (h + 1) * HEAD_DIM)
        packed_ref[h, :HEAD_DIM, :] = state[h]
        packed_ref[h, HEAD_DIM:, :] = jnp.broadcast_to(span_decay[:, lanes], (extra_rows, HEAD_DIM))


def mixer_finish(within_ref, qdec_ref, incoming_ref, gate_ref, scale_ref, w_ref, out_ref):
    channels = within_ref.shape[1]
    pieces = []
    for h in range(channels // HEAD_DIM):
        lanes = slice(h * HEAD_DIM, (h + 1) * HEAD_DIM)
        rec = within_ref[:, lanes] + dot(
            qdec_ref[:, lanes], incoming_ref[h, :HEAD_DIM, :].astype(bf16), NT
        )
        norm = lax.rsqrt(jnp.mean(rec * rec, axis=-1, keepdims=True) + 1e-06)
        gate = gate_ref[:, lanes].astype(f32)
        pieces.append((rec * norm * scale_ref[:, lanes] * (gate * sigmoid(gate))).astype(bf16))
    out_ref[...] = dot(jnp.concatenate(pieces, axis=1), w_ref[...]).astype(bf16)


def shifted(step, x):
    size = lax.axis_size("ep")
    links = [(i, i + step) for i in range(size - step)]
    early = lax.ppermute(x.astype(bf16), "ep", links).astype(f32)
    is_state = jnp.arange(x.shape[1])[None, :, None] < HEAD_DIM
    return jnp.where(lax.axis_index("ep") >= step, early, jnp.where(is_state, 0.0, 1.0))


def joined(step, late):
    early = shifted(step, late)
    is_state = jnp.arange(late.shape[1])[None, :, None] < HEAD_DIM
    decay = late[:, HEAD_DIM : HEAD_DIM + 1, :]
    return early * decay + jnp.where(is_state, late, 0.0)


def mixer_begin(query, forget, values, gap, extra):
    tokens, channels = query.shape
    heads = channels // HEAD_DIM
    within, qdec, packed = pl.pallas_call(
        mixer_local,
        name="mixer_local",
        out_shape=(
            jax.ShapeDtypeStruct((tokens, channels), f32),
            jax.ShapeDtypeStruct((tokens, channels), bf16),
            jax.ShapeDtypeStruct((heads, HEAD_DIM + 16, HEAD_DIM), f32),
        ),
    )(query, forget, values, extra, gap[None, :])
    return within, qdec, joined(1, shifted(1, packed))


def mixer_end(within, qdec, state, output_gate, head_scale, matrix):
    step = 2
    while step < lax.axis_size("ep") - 1:
        state = joined(step, state)
        step *= 2
    mixed = pl.pallas_call(
        mixer_finish,
        name="mixer_finish",
        out_shape=jax.ShapeDtypeStruct((within.shape[0], matrix.shape[1]), bf16),
    )(within, qdec, state, output_gate, head_scale[None, :], matrix)
    return lax.psum_scatter(mixed, "tp", scatter_dimension=0, tiled=True)


def dispatch(experts, capacity, place_ref, x_ref, own_ref, scale_ref, routes_ref, out_ref, slot_ref):
    tokens = x_ref.shape[0]
    x = x_ref[...].astype(f32)
    mean = jnp.mean(x, axis=-1, keepdims=True)
    centred = x - mean
    norm = lax.rsqrt(jnp.mean(centred * centred, axis=-1, keepdims=True) + 1e-05)
    own = ((own_ref[...].astype(f32) - mean) * norm * scale_ref[...]).astype(bf16)
    names = lax.broadcasted_iota(jnp.int32, (max(experts, 16), tokens), 0)
    first, second = routes_ref[0:1, :], routes_ref[1:2, :]
    is_first, is_second = names == first, names == second
    chosen = (is_first | is_second).astype(f32)
    before = (
        lax.broadcasted_iota(jnp.int32, (tokens, tokens), 0)
        < lax.broadcasted_iota(jnp.int32, (tokens, tokens), 1)
    ).astype(f32)
    position = dot(chosen.astype(bf16), before.astype(bf16))
    part = capacity // CHUNKS

    def slot(is_one, route):
        pos = jnp.sum(jnp.where(is_one, position, 0.0), axis=0, keepdims=True).astype(jnp.int32)
        chunk = sum((pos >= part * i).astype(jnp.int32) for i in range(1, CHUNKS))
        return (chunk * experts + route) * part + pos - chunk * part

    slot_first, slot_second = slot(is_first, first), slot(is_second, second)
    slots = lax.broadcasted_iota(jnp.int32, (out_ref.shape[0], tokens), 0)
    pick = jnp.where((slots == slot_first) | (slots == slot_second), 1.0, 0.0).astype(bf16)
    out_ref[...] = dot(pick, own).astype(bf16)
    which = lax.broadcasted_iota(jnp.int32, slot_ref.shape, 0)
    slot_ref[...] = jnp.where(which == 0, slot_first, slot_second)


def combine(slot_ref, scores_ref, *refs):
    out_ref, back = refs[-1], refs[:-1]
    first = sigmoid(scores_ref[:, 0:1] - scores_ref[:, 1:2])
    tokens = out_ref.shape[0]
    rows = back[0].shape[0]
    parts = []
    for k in range(2):
        total = None
        for c, ref in enumerate(back):
            slots = lax.broadcasted_iota(jnp.int32, (rows, tokens), 0) + c * rows
            pick = jnp.where(slots == slot_ref[k : k + 1, :], 1.0, 0.0).astype(bf16)
            term = dot(pick, ref[...], TN)
            total = term if total is None else total + term
        parts.append(total)
    out_ref[...] = (parts[0] * first + parts[1] * (1.0 - first)).astype(bf16)


def exchange(x, axis):
    return lax.all_to_all(x, axis, split_axis=0, concat_axis=0, tiled=True)


def expert_half(state, x, scale, routes, scores, gate_w, up_w, down_w):
    tokens, channels = x.shape
    experts, groups = lax.axis_size("ep"), lax.axis_size("tp")
    capacity = 3 * tokens // experts
    width = channels // groups
    total_slots = experts * capacity
    outgoing, slot = pl.pallas_call(
        functools.partial(dispatch, experts, capacity),
        name="dispatch",
        grid_spec=pltpu.PrefetchScalarGridSpec(
            num_scalar_prefetch=1,
            grid=(1,),
            in_specs=[
                pl.BlockSpec((tokens, channels), lambda i, s: (0, 0)),
                pl.BlockSpec((tokens, width), lambda i, s: (0, s[0])),
                pl.BlockSpec((1, width), lambda i, s: (0, s[0])),
                pl.BlockSpec((2, tokens), lambda i, s: (0, 0)),
            ],
            out_specs=[
                pl.BlockSpec((total_slots, width), lambda i, s: (0, 0)),
                pl.BlockSpec((8, tokens), lambda i, s: (0, 0)),
            ],
        ),
        out_shape=(
            jax.ShapeDtypeStruct((total_slots, width), bf16),
            jax.ShapeDtypeStruct((8, tokens), jnp.int32),
        ),
    )(lax.axis_index("tp").astype(jnp.int32)[None], x, x, scale[None, :], routes.T)
    rows = total_slots // CHUNKS
    back = []
    for c in range(CHUNKS):
        arrived = exchange(outgoing[c * rows : (c + 1) * rows], "ep")
        features = lax.all_gather(arrived, "tp", axis=1, tiled=True)
        features, state = lax.optimization_barrier((features, state))
        gate, up = dot(features, gate_w[0]), dot(features, up_w[0])
        hidden = (jax.nn.silu(gate) * up).astype(bf16)
        result = dot(hidden, down_w[0], NT).astype(bf16)
        summed = lax.psum_scatter(result, "tp", scatter_dimension=1, tiled=True)
        back.append(exchange(summed, "ep"))
    combined = pl.pallas_call(
        combine, name="combine", out_shape=jax.ShapeDtypeStruct((tokens, width), bf16)
    )(slot, scores, *back)
    return state, combined


def body(q, f, v, og, gap, extra, head_scale, matrix, x, scale, routes, scores, gw, uw, dw):
    within, qdec, state = mixer_begin(q, f, v, gap, extra)
    state, expert_out = expert_half(state, x, scale, routes, scores, gw, uw, dw)
    mixer_output_rows = mixer_end(within, qdec, state, og, head_scale, matrix)
    return (mixer_output_rows, expert_out)


def solution(mesh):
    wide, experts = P("ep", "tp"), P("ep", None, "tp")
    rows = P("ep", None)
    mixer_specs = (wide, wide, wide, wide, P("tp"), wide, P("tp"), P("tp", None))
    expert_specs = (rows, P(), rows, rows, experts, experts, experts)
    return jax.shard_map(
        body,
        mesh=mesh,
        in_specs=mixer_specs + expert_specs,
        out_specs=(P(("ep", "tp"), None), P("ep", "tp")),
        check_vma=False,
    )
```
